256 devices in a mesh: sp: 64 (over z, x, core), tp: 4 (over y).
Axes of the slice: x: 4, y: 4, z: 8, core: 2. Of those that a mesh axis runs over, the one named last changes fastest.
Arguments:
- hidden_in: bfloat16 [4096, 2048], P(('sp', 'tp')), may hold values from -6 to 6
- pre_gain: float32 [2048], replicated, may hold values from 0.5 to 1.5
- w_query: bfloat16 [2048, 1024], P(None, 'tp'), may hold values from -0.4375 to 0.4375
- w_key: bfloat16 [2048, 1024], P(None, 'tp'), may hold values from -0.125 to 0.125
- w_value: bfloat16 [2048, 1024], P(None, 'tp'), may hold values from -0.125 to 0.125
- stick_offset: float32 [8], P('tp'), may hold values from -15.2 to -14.2
- w_glu_a: bfloat16 [2048, 1024], P(None, 'tp'), may hold values from -0.125 to 0.125
- w_glu_b: bfloat16 [2048, 1024], P(None, 'tp'), may hold values from -0.125 to 0.125
- w_gate_attn: bfloat16 [2048, 2048], P(None, 'tp'), may hold values from -0.125 to 0.125
- w_gate_conv: bfloat16 [2048, 2048], P(None, 'tp'), may hold values from -0.125 to 0.125
- conv_taps: float32 [31, 1024], P(None, 'tp'), may hold values from -1 to 1
- conv_bias: float32 [1024], P('tp'), may hold values from -0.6 to 0.6
- norm_gain: float32 [1024], P('tp'), may hold values from 0.5 to 1.5
- norm_shift: float32 [1024], P('tp'), may hold values from -0.6 to 0.6
- w_attn_out: bfloat16 [1024, 2048], P('tp'), may hold values from -0.4375 to 0.4375
- w_conv_out: bfloat16 [1024, 2048], P('tp'), may hold values from -0.1875 to 0.1875
- post_gain: float32 [2048], P('tp'), may hold values from 0.5 to 1.5
Outputs:
- mixed: bfloat16 [4096, 2048], P('sp', 'tp')
The draws below stay inside these ranges and needn't reach their ends.
All inputs are finite; a program needn't handle non-finite values.
Results may differ from the reference program's by a relative error of at most 0.015.
Values may be sent and summed in bfloat16 or wider, within the bound.
No kernel may reach another device: no remote copies, remote signals or barrier semaphores. Data moves between devices by JAX's collectives and lax.ppermute only.
A program may use at most 64 MiB of HBM per device.

```python
import math
import jax
import jax.numpy as jnp
from jax import lax

D = 2048
HEADS = 8
HEAD_DIM = 128
CONV_CH = 1024
WIDTH = 31
TOK_DEV = 64
TOKENS = 4096
N_SP = 64


def block_scale(stream_key, dims, shards, least, top_value):
    gain = 1.0
    for position, blocks in shards:
        steps = jax.random.uniform(jax.random.fold_in(jax.random.fold_in(stream_key, 6), position), (blocks,), jnp.float32, least / len(shards), top_value / len(shards))
        gain = gain * jnp.repeat(jnp.exp(steps), dims[position] // blocks).reshape((-1,) + (1,) * (len(dims) - 1 - position))
    return gain


def centred(rng, extent, deviation, limit, shards=(), held_as=jnp.bfloat16):
    result = jax.random.normal(rng, extent, jnp.float32) * deviation
    if len(shards) > 0:
        result = block_scale(rng, extent, shards, -0.22, 0.18) * result
    return jnp.clip(result, min=-limit, max=limit).astype(held_as)


def setup_inputs(seed: int = 0) -> dict:
    key_of = jax.random.split(jax.random.key(seed), 18)
    return {
        "hidden_in": centred(key_of[0], (TOKENS, D), 1.0, 6.0, ((0, 256),)),
        "pre_gain": jnp.clip(1.0 + 0.1 * jax.random.normal(key_of[1], (D,), jnp.float32), 0.5, 1.5),
        "w_query": centred(key_of[2], (D, HEADS * HEAD_DIM), (D // 12) ** -0.5, 0.4375, ((1, 4),)),
        "w_key": centred(key_of[3], (D, HEADS * HEAD_DIM), D ** -0.5, 0.125, ((1, 4),)),
        "w_value": centred(key_of[4], (D, HEADS * HEAD_DIM), D ** -0.5, 0.125, ((1, 4),)),
        "stick_offset": jnp.clip(-15.2 + 1.0 * jax.random.uniform(key_of[5], (HEADS,), jnp.float32) ** block_scale(key_of[5], (HEADS,), ((0, 4),), -0.2, 0.2), -15.2, -14.2),
        "w_glu_a": centred(key_of[6], (D, CONV_CH), D ** -0.5, 0.125, ((1, 4),)),
        "w_glu_b": centred(key_of[7], (D, CONV_CH), D ** -0.5, 0.125, ((1, 4),)),
        "w_gate_attn": centred(key_of[8], (D, D), D ** -0.5, 0.125, ((1, 4),)),
        "w_gate_conv": centred(key_of[9], (D, D), D ** -0.5, 0.125, ((1, 4),)),
        "conv_taps": centred(key_of[10], (WIDTH, CONV_CH), WIDTH ** -0.5, 1.0, ((1, 4),), jnp.float32),
        "conv_bias": centred(key_of[11], (CONV_CH,), 0.1, 0.6, ((0, 4),), jnp.float32),
        "norm_gain": jnp.clip(1.0 + 0.1 * jax.random.normal(key_of[12], (CONV_CH,), jnp.float32), 0.5, 1.5),
        "norm_shift": centred(key_of[13], (CONV_CH,), 0.1, 0.6, ((0, 4),), jnp.float32),
        "w_attn_out": centred(key_of[14], (HEADS * HEAD_DIM, D), (HEADS * HEAD_DIM // 6) ** -0.5, 0.4375, ((0, 4),)),
        "w_conv_out": centred(key_of[15], (CONV_CH, D), CONV_CH ** -0.5, 0.1875, ((0, 4),)),
        "post_gain": jnp.clip(1.0 + 0.1 * jax.random.normal(key_of[16], (D,), jnp.float32), 0.5, 1.5),
    }


epsilon = 1e-06

def held_bf16(values):
    return lax.optimization_barrier(values.astype(jnp.bfloat16))

def reference(hidden_in, pre_gain, w_query, w_key, w_value, stick_offset, w_glu_a, w_glu_b, w_gate_attn, w_gate_conv, conv_taps, conv_bias, norm_gain, norm_shift, w_attn_out, w_conv_out, post_gain):
    values = hidden_in.astype(jnp.float32)
    inverse = lax.rsqrt(lax.optimization_barrier(jnp.mean(values * values, axis=1, keepdims=True)) + epsilon)
    normed = (values * inverse * pre_gain).astype(jnp.bfloat16)

    def project(weight):
        return held_bf16(jnp.dot(normed, weight, preferred_element_type=jnp.float32))
    queries = project(w_query).astype(jnp.float32).reshape(TOKENS, HEADS, HEAD_DIM)
    key_rows = project(w_key).astype(jnp.float32).reshape(TOKENS, HEADS, HEAD_DIM)
    value_rows = project(w_value).astype(jnp.float32).reshape(TOKENS, HEADS, HEAD_DIM)
    glu_left = project(w_glu_a).astype(jnp.float32)
    glu_right = project(w_glu_b).astype(jnp.float32)
    gate_attn = project(w_gate_attn).astype(jnp.float32)
    gate_conv = project(w_gate_conv).astype(jnp.float32)
    positions = jnp.arange(TOKENS, dtype=jnp.int32)

    def attend_block(block_start):
        query_block = lax.dynamic_slice_in_dim(queries, block_start, TOK_DEV, 0)
        scores = jnp.einsum('thd,shd->hts', query_block, key_rows, precision=lax.Precision.HIGHEST)
        scores = scores / math.sqrt(HEAD_DIM) + stick_offset[:, None, None]
        query_pos = block_start + jnp.arange(TOK_DEV, dtype=jnp.int32)
        causal = (positions[None, :] < query_pos[:, None])[None]
        log_rest = jnp.where(causal, jax.nn.log_sigmoid(-scores), 0.0)
        suffix = lax.cumsum(log_rest, axis=2, reverse=True) - log_rest
        weights = jnp.where(causal, jnp.exp(jax.nn.log_sigmoid(scores) + suffix), 0.0)
        return jnp.einsum('hts,shd->thd', weights, value_rows, precision=lax.Precision.HIGHEST)
    starts = jnp.arange(N_SP, dtype=jnp.int32) * TOK_DEV
    attended = lax.map(attend_block, starts).reshape(TOKENS, HEADS * HEAD_DIM).astype(jnp.bfloat16)
    attn_branch = held_bf16(jnp.dot(attended, w_attn_out, preferred_element_type=jnp.float32)).astype(jnp.float32)
    gated_in = held_bf16(glu_left * jax.nn.sigmoid(glu_right)).astype(jnp.float32)
    padded = jnp.pad(gated_in, ((WIDTH - 1, 0), (0, 0)))
    convolved = lax.conv_general_dilated(padded[None], conv_taps.reshape(WIDTH, 1, CONV_CH), (1,), 'VALID', dimension_numbers=('NWC', 'WIO', 'NWC'), feature_group_count=CONV_CH, precision=lax.Precision.HIGHEST)[0] + conv_bias
    mean_row = lax.optimization_barrier(jnp.mean(convolved, axis=1, keepdims=True))
    centered = convolved - mean_row
    spread = lax.optimization_barrier(jnp.mean(centered * centered, axis=1, keepdims=True))
    conv_normed = jax.nn.silu(centered * lax.rsqrt(spread + epsilon) * norm_gain + norm_shift).astype(jnp.bfloat16)
    conv_branch = held_bf16(jnp.dot(conv_normed, w_conv_out, preferred_element_type=jnp.float32)).astype(jnp.float32)
    merged = jax.nn.sigmoid(gate_attn) * attn_branch + jax.nn.sigmoid(gate_conv) * conv_branch
    squares = lax.optimization_barrier(jnp.mean(merged * merged, axis=1, keepdims=True))
    return (merged * lax.rsqrt(squares + epsilon) * post_gain).astype(jnp.bfloat16)
```

```python
import math

import jax
import jax.numpy as jnp
from jax import lax
from jax.experimental import pallas as pl
from jax.experimental.pallas import tpu as pltpu
from jax.sharding import Mesh
from jax.sharding import PartitionSpec as P

D = 2048
HEAD_DIM = 128
CONV_CH = 1024
WIDTH = 31
HALO = 32
SP = ("zh", "zl", "x", "c")
SP_TP = ("zh", "zl", "x", "c", "tp")
N_ZH = 4
N_TP = 4
LOG2E = math.log2(math.e)
BF16 = jnp.bfloat16
F32 = jnp.float32
epsilon = 1e-06
MIB = 1024 * 1024


def dot(a, b):
    return jnp.dot(a, b, preferred_element_type=F32)


def call(body, outs, args, name, scratch=(), vmem=24, flops=0):
    specs = [
        pl.BlockSpec(memory_space=pltpu.SMEM) if kind == "smem" else pl.BlockSpec(memory_space=pltpu.VMEM)
        for kind, _ in args
    ]
    return pl.pallas_call(
        body,
        out_shape=[jax.ShapeDtypeStruct(shape, dtype) for shape, dtype in outs],
        in_specs=specs,
        out_specs=[pl.BlockSpec(memory_space=pltpu.VMEM) for _ in outs],
        scratch_shapes=list(scratch),
        compiler_params=pltpu.CompilerParams(vmem_limit_bytes=vmem * MIB),
        cost_estimate=pl.CostEstimate(flops=flops, transcendentals=0, bytes_accessed=0),
        name=name,
    )(*[array for _, array in args])


def rotated(x, distance):
    return lax.ppermute(x, "tp", [(i, (i + distance) % N_TP) for i in range(N_TP)])


def to_rotated(pieces):
    return [rotated(piece, d + 1) for d, piece in enumerate(pieces)]


def qkv_body(x0, x1, x2, x3, gain, wq, wk, wv, kv_out, q_out, normed_out, rows):
    me = lax.axis_index("tp")
    for d, ref in enumerate((x0, x1, x2, x3)):
        source = lax.rem(me + N_TP - d, N_TP)
        rows[pl.ds(pl.multiple_of(source * 16, 16), 16), :] = ref[...]
    values = rows[...].astype(F32)
    inverse = lax.rsqrt(jnp.mean(values * values, axis=1, keepdims=True) + epsilon)
    normed = (values * inverse * gain[...]).astype(BF16)
    normed_out[...] = normed
    keys = dot(normed, wk[...]).astype(BF16)
    vals = dot(normed, wv[...]).astype(BF16)
    for i in range(kv_out.shape[0]):
        kv_out[i, :, 0:256] = keys
        kv_out[i, :, 256:512] = vals
    q_out[...] = dot(normed, wq[...]).astype(BF16)


def glu_body(normed_ref, wa, wb, gated_out, tail_out):
    normed = normed_ref[...]
    left = dot(normed, wa[...]).astype(BF16).astype(F32)
    right = dot(normed, wb[...]).astype(BF16).astype(F32)
    gated = (left * jax.nn.sigmoid(right)).astype(BF16)
    gated_out[...] = gated
    tail_out[...] = gated[gated.shape[0] - HALO :, :]


def gates_body(normed_ref, wa, wc, ga_out, gc_out):
    normed = normed_ref[...]
    ga_out[...] = jax.nn.sigmoid(dot(normed, wa[...]).astype(BF16).astype(F32))
    gc_out[...] = jax.nn.sigmoid(dot(normed, wc[...]).astype(BF16).astype(F32))


def conv_body(gated_ref, tail_ref, taps, bias, conv_out, stat_out, padded):
    rows = gated_ref.shape[0]
    padded[0:HALO, :] = tail_ref[...].astype(F32)
    padded[HALO : HALO + rows, :] = gated_ref[...].astype(F32)
    total = jnp.broadcast_to(bias[...], (rows, bias.shape[1]))
    first = HALO - (WIDTH - 1)
    for i in range(WIDTH):
        total = total + taps[i : i + 1, :] * padded[first + i : first + i + rows, :]
    conv_out[...] = total
    mean = jnp.mean(total, axis=1, keepdims=True)
    centered = total - mean
    squares = jnp.sum(centered * centered, axis=1, keepdims=True)
    lane = lax.broadcasted_iota(jnp.int32, (rows, 128), 1)
    stat_out[...] = jnp.where(lane < 64, mean, squares)


def conv_out_body(conv_ref, s0, s1, s2, s3, gain, shift, weight, own_out, p1, p2, p3):
    stats = [s[...] for s in (s0, s1, s2, s3)]
    means = [s[:, 0:1] for s in stats]
    mean = (means[0] + means[1] + means[2] + means[3]) * (1.0 / N_TP)
    spread = 0.0
    for s, m in zip(stats, means):
        spread = spread + s[:, 64:65] + (m - mean) * (m - mean) * (CONV_CH // N_TP)
    spread = spread * (1.0 / CONV_CH)
    scaled = (conv_ref[...] - mean) * lax.rsqrt(spread + epsilon) * gain[...] + shift[...]
    normed = (scaled * jax.nn.sigmoid(scaled)).astype(BF16)
    project_out(normed, weight, own_out, (p1, p2, p3))


def project_out(rows, weight, own_out, pieces):
    me = lax.axis_index("tp")
    width = own_out.shape[1]
    for d, ref in enumerate((own_out,) + tuple(pieces)):
        target = lax.rem(me + d, N_TP)
        columns = pl.ds(pl.multiple_of(target * width, width), width)
        ref[...] = dot(rows, weight[:, columns]).astype(ref.dtype)


def attend_body(offset, q0, q1, q2, q3, mine, other, acc_out, rest_out, m1, m2, m3):
    core = lax.axis_index("c")
    rows = q0.shape[0]
    blocks = mine.shape[0]
    position = (lax.axis_index("zl") * 4 + lax.axis_index("x")) * 128 + core * 64
    query_pos = position + lax.broadcasted_iota(jnp.int32, (rows, 128), 0)
    index = lax.broadcasted_iota(jnp.int32, (1, 128), 1)
    place = lax.rem(index + core * 64, 128)
    row_index = lax.broadcasted_iota(jnp.int32, (128, 256), 0)
    col_index = lax.broadcasted_iota(jnp.int32, (128, 256), 1)
    row_place = lax.rem(row_index + core * 64, 128)
    col_place = lax.rem(col_index + core * 64, 128)
    suffix = jnp.where((col_index >= 128) | (row_place >= col_place), 1.0, 0.0).astype(BF16)
    scale = LOG2E / math.sqrt(HEAD_DIM)
    later = jnp.full((3 * rows, 128), True)
    for h in range(2):
        lanes = slice(h * 128, h * 128 + 128)
        value_lanes = slice(256 + h * 128, 256 + h * 128 + 128)
        queries = jnp.concatenate([q[:, lanes] for q in (q0, q1, q2, q3)], axis=0)
        shift = offset[h] * LOG2E
        rest = jnp.zeros((4 * rows, 128), F32)
        acc = jnp.zeros((4 * rows, 128), F32)
        for b in reversed(range(blocks)):
            keys = jnp.concatenate([mine[b, :, lanes], other[b, :, lanes]], axis=0)
            vals = jnp.concatenate([mine[b, :, value_lanes], other[b, :, value_lanes]], axis=0)
            scores = lax.dot_general(queries, keys, (((1,), (1,)), ((), ())), preferred_element_type=F32)
            scores = scores * scale + shift
            soft = jnp.maximum(scores, 0.0) + jnp.log2(1.0 + jnp.exp2(-jnp.abs(scores)))
            own_causal = (b * 128 + place) < query_pos
            soft = jnp.concatenate([jnp.where(own_causal, soft[:rows], 0.0), soft[rows:]], axis=0)
            high = soft.astype(BF16)
            low = (soft - high.astype(F32)).astype(BF16)
            sums = dot(high, suffix) + dot(low, suffix)
            stick = jnp.exp2(scores - sums[:, 0:128] - rest)
            stick = jnp.concatenate([jnp.where(own_causal, stick[:rows], 0.0), stick[rows:]], axis=0)
            acc = acc + dot(stick.astype(BF16), vals)
            rest = rest + sums[:, 128:256]
        acc_out[:, lanes] = acc[:rows]
        rest_out[:, lanes] = rest[:rows]
        lane = lax.broadcasted_iota(jnp.int32, (rows, 64), 1)
        for d, ref in ((1, m1), (2, m2), (3, m3)):
            part = slice(d * rows, d * rows + rows)
            ref[:, lanes] = acc[part].astype(BF16)
            total = rest[part][:, 0:64]
            t1 = total.astype(BF16).astype(F32)
            t2 = (total - t1).astype(BF16).astype(F32)
            t3 = total - t1 - t2
            ref[:, 256 + h * 64 : 320 + h * 64] = jnp.where(lane == 0, t1, jnp.where(lane == 1, t2, t3)).astype(BF16)


def merge_body(acc_ref, rest_ref, m1, m2, m3, weight, own_out, p1, p2, p3):
    heads = []
    for h in range(2):
        lanes = slice(h * 128, h * 128 + 128)
        outside = rest_ref[:, lanes]
        total = acc_ref[:, lanes]
        for ref in (m1, m2, m3):
            total = total + jnp.exp2(-outside) * ref[:, lanes].astype(F32)
            sent = ref[:, 256 + h * 64 : 320 + h * 64].astype(F32)
            outside = outside + (sent[:, 0:1] + sent[:, 1:2] + sent[:, 2:3])
        heads.append(total.astype(BF16))
    project_out(jnp.concatenate(heads, axis=1), weight, own_out, (p1, p2, p3))


def gather_body(a0, a1, a2, a3, c0, c1, c2, c3, ga, gc, merged_out, stat_out):
    attn = (a0[...] + a1[...].astype(F32) + a2[...].astype(F32) + a3[...].astype(F32)).astype(BF16).astype(F32)
    conv = (c0[...] + c1[...].astype(F32) + c2[...].astype(F32) + c3[...].astype(F32)).astype(BF16).astype(F32)
    merged = ga[...] * attn + gc[...] * conv
    merged_out[...] = merged
    stat_out[...] = jnp.broadcast_to(jnp.sum(merged * merged, axis=1, keepdims=True), stat_out.shape)


def final_body(merged, s0, s1, s2, s3, gain, out):
    squares = (s0[...] + s1[...] + s2[...] + s3[...])[:, 0:1] * (1.0 / D)
    out[...] = (merged[...] * lax.rsqrt(squares + epsilon) * gain[...]).astype(BF16)


def on_device(
    hidden_in,
    pre_gain,
    w_query,
    w_key,
    w_value,
    stick_offset,
    w_glu_a,
    w_glu_b,
    w_gate_attn,
    w_gate_conv,
    conv_taps,
    conv_bias,
    norm_gain,
    norm_shift,
    w_attn_out,
    w_conv_out,
    post_gain,
):
    def v(x):
        return ("vmem", x)

    rows = 64
    pieces = [hidden_in] + to_rotated([hidden_in] * 3)
    kv, q, normed = call(
        qkv_body,
        [((8, rows, 512), BF16), ((rows, 256), BF16), ((rows, D), BF16)],
        [v(p) for p in pieces] + [v(pre_gain.reshape(1, D)), v(w_query), v(w_key), v(w_value)],
        "qkv",
        scratch=[pltpu.VMEM((rows, D), BF16)],
        flops=2 * rows * D * 768,
    )
    kv_mine = lax.all_to_all(kv, ("zl", "x"), 0, 0)
    visitors = [
        lax.ppermute(q, "zh", [(i, i - d) for i in range(d, N_ZH)]) for d in range(1, N_ZH)
    ]
    gated, tail = call(
        glu_body,
        [((rows, 256), BF16), ((HALO, 256), BF16)],
        [v(normed), v(w_glu_a), v(w_glu_b)],
        "glu",
        flops=2 * rows * D * 512,
    )
    before = lax.ppermute(tail, SP, [(i, i + 1) for i in range(lax.axis_size(SP) - 1)])
    gate_a, gate_c = call(
        gates_body,
        [((rows, 512), F32), ((rows, 512), F32)],
        [v(normed), v(w_gate_attn), v(w_gate_conv)],
        "gates",
        flops=2 * rows * D * 1024,
    )
    convolved, stat = call(
        conv_body,
        [((rows, 256), F32), ((rows, 128), F32)],
        [v(gated), v(before), v(conv_taps), v(conv_bias.reshape(1, 256))],
        "conv",
        scratch=[pltpu.VMEM((rows + HALO, 256), F32)],
        flops=2 * rows * 256 * 31 * 40,
    )
    stats = [stat] + to_rotated([stat] * 3)
    conv_pieces = call(
        conv_out_body,
        [((rows, 512), F32)] + [((rows, 512), BF16)] * 3,
        [v(convolved)]
        + [v(s) for s in stats]
        + [v(norm_gain.reshape(1, 256)), v(norm_shift.reshape(1, 256)), v(w_conv_out)],
        "conv_out",
        flops=2 * rows * 256 * D,
    )
    conv_sums = [conv_pieces[0]] + to_rotated(conv_pieces[1:])

    kv_other = lax.ppermute(kv_mine, "c", [(0, 1), (1, 0)])
    acc, rest, *messages = call(
        attend_body,
        [((rows, 256), F32), ((rows, 256), F32)] + [((rows, 384), BF16)] * 3,
        [("smem", stick_offset), v(q)] + [v(x) for x in visitors] + [v(kv_mine), v(kv_other)],
        "attend",
        flops=2 * 2 * 256 * 1024 * 128 * 2,
    )
    returned = [
        lax.ppermute(m, "zh", [(i, i + d + 1) for i in range(N_ZH - d - 1)])
        for d, m in enumerate(messages)
    ]
    attn_pieces = call(
        merge_body,
        [((rows, 512), F32)] + [((rows, 512), BF16)] * 3,
        [v(acc), v(rest)] + [v(m) for m in returned] + [v(w_attn_out)],
        "merge",
        flops=2 * rows * 256 * D,
    )
    attn_sums = [attn_pieces[0]] + to_rotated(attn_pieces[1:])
    merged, square = call(
        gather_body,
        [((rows, 512), F32), ((rows, 128), F32)],
        [v(x) for x in attn_sums] + [v(x) for x in conv_sums] + [v(gate_a), v(gate_c)],
        "gather",
        flops=1000000,
    )
    squares = [square] + to_rotated([square] * 3)
    (out,) = call(
        final_body,
        [((rows, 512), BF16)],
        [v(merged)] + [v(s) for s in squares] + [v(post_gain.reshape(1, 512))],
        "final",
        flops=1000000,
    )
    return out


def solution(mesh):
    torus = Mesh(mesh.devices.reshape(4, 2, 4, 2, mesh.shape["tp"]), SP_TP)
    return jax.shard_map(
        on_device,
        mesh=torus,
        in_specs=(
            P(SP_TP, None),
            P(),
            P(None, "tp"),
            P(None, "tp"),
            P(None, "tp"),
            P("tp"),
            P(None, "tp"),
            P(None, "tp"),
            P(None, "tp"),
            P(None, "tp"),
            P(None, "tp"),
            P("tp"),
            P("tp"),
            P("tp"),
            P("tp", None),
            P("tp", None),
            P("tp"),
        ),
        out_specs=P(SP, "tp"),
        check_vma=False,
    )
```

```python
import math

import jax
import jax.numpy as jnp
from jax import lax
from jax.experimental import pallas as pl
from jax.experimental.pallas import tpu as pltpu
from jax.sharding import Mesh
from jax.sharding import PartitionSpec as P

D = 2048
HEAD_DIM = 128
CONV_CH = 1024
WIDTH = 31
HALO = 32
SP = ("zh", "zl", "x", "c")
SP_TP = ("zh", "zl", "x", "c", "tp")
N_ZH = 4
N_TP = 4
LOG2E = math.log2(math.e)
BF16 = jnp.bfloat16
F32 = jnp.float32
epsilon = 1e-06
MIB = 1024 * 1024
LOAD_PARTS = 4


def dot(a, b):
    return jnp.dot(a, b, preferred_element_type=F32)


def call(body, outs, args, scratch=(), vmem=8, flops=0, out_space=jax.ShapeDtypeStruct):
    spaces = {"smem": pltpu.SMEM, "vmem": pltpu.VMEM, "hbm": pltpu.HBM}
    specs = [pl.BlockSpec(memory_space=spaces[kind]) for kind, _ in args]
    return pallas_call(body, outs, specs, args, scratch, vmem, flops, out_space)


def pallas_call(body, outs, specs, args, scratch, vmem, flops, out_space):
    return pl.pallas_call(
        body,
        out_shape=[out_space(shape, dtype) for shape, dtype in outs],
        in_specs=specs,
        out_specs=[pl.BlockSpec(memory_space=pltpu.VMEM) for _ in outs],
        scratch_shapes=list(scratch),
        compiler_params=pltpu.CompilerParams(vmem_limit_bytes=vmem * MIB),
        cost_estimate=pl.CostEstimate(flops=flops, transcendentals=0, bytes_accessed=0),
    )(*[array for _, array in args])


def to_rotated(pieces):
    return [lax.ppermute(piece, "tp", [(i, (i + d) % N_TP) for i in range(N_TP)]) for d, piece in enumerate(pieces, 1)]


def load_body(*refs):
    count = (len(refs) - 1) // 2
    sems = refs[-1]
    copies = []
    for source, target in zip(refs[:count], refs[count:-1]):
        parts = LOAD_PARTS if source.shape[0] >= 256 else 1
        rows = source.shape[0] // parts
        for i in range(parts):
            part = pl.ds(i * rows, rows)
            copies.append(pltpu.make_async_copy(source.at[part], target.at[part], sems.at[len(copies)]))
    for copy in copies:
        copy.start()
    for copy in copies:
        copy.wait()


def loaded(arrays):
    arrays = [pltpu.with_memory_space_constraint(x, pltpu.HBM) for x in arrays]
    return call(
        load_body,
        [(x.shape, x.dtype) for x in arrays],
        [("hbm", x) for x in arrays],
        scratch=[pltpu.SemaphoreType.DMA((LOAD_PARTS * len(arrays),))],
        flops=10000000,
        out_space=pltpu.VMEM,
    )


def qkv_body(x0, x1, x2, x3, gain, wq, wk, wv, kv_out, q_out, normed_out, rows):
    me = lax.axis_index("tp")
    for d, ref in enumerate((x0, x1, x2, x3)):
        source = lax.rem(me + N_TP - d, N_TP)
        rows[pl.ds(pl.multiple_of(source * 16, 16), 16), :] = ref[...]
    values = rows[...].astype(F32)
    inverse = lax.rsqrt(jnp.mean(values * values, axis=1, keepdims=True) + epsilon)
    normed = (values * inverse * gain[...]).astype(BF16)
    normed_out[...] = normed
    keys = dot(normed, wk[...]).astype(BF16)
    vals = dot(normed, wv[...]).astype(BF16)
    for i in range(kv_out.shape[0]):
        kv_out[i, :, 0:256] = keys
        kv_out[i, :, 256:512] = vals
    q_out[...] = dot(normed, wq[...]).astype(BF16)


def glu_body(normed_ref, wa, wb, gated_out, tail_out):
    normed = normed_ref[...]
    left = dot(normed, wa[...]).astype(BF16).astype(F32)
    right = dot(normed, wb[...]).astype(BF16).astype(F32)
    gated = (left * jax.nn.sigmoid(right)).astype(BF16)
    gated_out[...] = gated
    tail_out[...] = gated[gated.shape[0] - HALO :, :]


def gates_body(normed_ref, wa, wc, ga_out, gc_out, held, sems):
    rows = D // LOAD_PARTS
    copies = []
    for i in range(LOAD_PARTS):
        part = pl.ds(i * rows, rows)
        for j, source in enumerate((wa, wc)):
            copies.append(pltpu.make_async_copy(source.at[part], held.at[j, part], sems.at[len(copies)]))
    for copy in copies:
        copy.start()
    totals = [0.0, 0.0]
    for i in range(LOAD_PARTS):
        part = slice(i * rows, i * rows + rows)
        for j in range(2):
            copies[2 * i + j].wait()
            totals[j] = totals[j] + dot(normed_ref[:, part], held[j, part, :])
    ga_out[...] = jax.nn.sigmoid(totals[0].astype(BF16).astype(F32))
    gc_out[...] = jax.nn.sigmoid(totals[1].astype(BF16).astype(F32))


def conv_body(gated_ref, tail_ref, taps, bias, conv_out, stat_out, padded):
    rows = gated_ref.shape[0]
    padded[0:HALO, :] = tail_ref[...].astype(F32)
    padded[HALO : HALO + rows, :] = gated_ref[...].astype(F32)
    total = jnp.broadcast_to(bias[...], (rows, bias.shape[1]))
    first = HALO - (WIDTH - 1)
    for i in range(WIDTH):
        total = total + taps[i : i + 1, :] * padded[first + i : first + i + rows, :]
    conv_out[...] = total
    mean = jnp.mean(total, axis=1, keepdims=True)
    centered = total - mean
    squares = jnp.sum(centered * centered, axis=1, keepdims=True)
    lane = lax.broadcasted_iota(jnp.int32, (rows, 128), 1)
    turned = jnp.transpose(jnp.where(lane < 4, mean, squares))
    stat_out[...] = turned[0:8, :]


def conv_norm_body(conv_ref, s0, s1, s2, s3, gain, shift, normed_out):
    stats = [s[...] for s in (s0, s1, s2, s3)]
    means = [s[0:4, :] for s in stats]
    mean = (means[0] + means[1] + means[2] + means[3]) * (1.0 / N_TP)
    spread = jnp.zeros_like(mean)
    for s, m in zip(stats, means):
        spread = spread + s[4:8, :] + (m - mean) * (m - mean) * (CONV_CH // N_TP)
    inverse = lax.rsqrt(spread * (1.0 / CONV_CH) + epsilon)
    columns = jnp.transpose(jnp.concatenate([mean, inverse], axis=0))
    mean = columns[:, 0:1]
    inverse = columns[:, 4:5]
    scaled = (conv_ref[...] - mean) * inverse * gain[...] + shift[...]
    normed_out[...] = (scaled * jax.nn.sigmoid(scaled)).astype(BF16)


def attend_body(offset, q0, q1, q2, q3, mine, other, acc_out, rest_out, m1, m2, m3):
    group = lax.axis_index("zh")
    visitors = ((q1, m1), (q2, m2), (q3, m3))
    for condition, count in ((group < N_ZH - 2, 3), (group == N_ZH - 2, 1), (group == N_ZH - 1, 0)):

        @pl.when(condition)
        def _():
            attend(offset, q0, visitors[:count], mine, other, acc_out, rest_out)


def attend(offset, q0, visitors, mine, other, acc_out, rest_out):
    core = lax.axis_index("c")
    rows = q0.shape[0]
    blocks = mine.shape[0]
    total_rows = rows * (1 + len(visitors))
    position = (lax.axis_index("zl") * 4 + lax.axis_index("x")) * 128 + core * 64
    query_pos = position + lax.broadcasted_iota(jnp.int32, (rows, 128), 0)
    index = lax.broadcasted_iota(jnp.int32, (1, 128), 1)
    place = lax.rem(index + core * 64, 128)
    row_index = lax.rem(lax.broadcasted_iota(jnp.int32, (256, 256), 0), 128)
    col_index = lax.broadcasted_iota(jnp.int32, (256, 256), 1)
    row_place = lax.rem(row_index + core * 64, 128)
    col_place = lax.rem(col_index + core * 64, 128)
    suffix = jnp.where((col_index >= 128) | (row_place >= col_place), 1.0, 0.0).astype(BF16)
    scale = LOG2E / math.sqrt(HEAD_DIM)

    tiles = range(blocks)
    span = [slice(b * 128, b * 128 + 128) for b in tiles]
    own_causal = [(b * 128 + place) < query_pos for b in tiles]

    def for_own(b, x):
        masked = jnp.where(own_causal[b], x[:rows], 0.0)
        return jnp.concatenate([masked, x[rows:]], axis=0) if visitors else masked

    for h in range(2):
        lanes = slice(h * 128, h * 128 + 128)
        value_lanes = slice(256 + h * 128, 256 + h * 128 + 128)
        queries = jnp.concatenate([q[:, lanes] for q in [q0] + [q for q, _ in visitors]], axis=0)
        keys = jnp.concatenate([ref[b, :, lanes] for b in tiles for ref in (mine, other)], axis=0)
        vals = jnp.concatenate([ref[b, :, value_lanes] for b in tiles for ref in (mine, other)], axis=0)
        scores = lax.dot_general(queries, keys, (((1,), (1,)), ((), ())), preferred_element_type=F32)
        scores = scores * scale + offset[h] * LOG2E
        soft = jnp.maximum(scores, 0.0) + jnp.log2(1.0 + jnp.exp2(-jnp.abs(scores)))
        split = []
        for b in tiles:
            part = for_own(b, soft[:, span[b]])
            high = part.astype(BF16)
            low = (part - high.astype(F32)).astype(BF16)
            split.append(jnp.concatenate([high, low], axis=1))
        sums = dot(jnp.concatenate(split, axis=0), suffix)
        sums = [sums[b * total_rows : (b + 1) * total_rows] for b in tiles]
        rest = jnp.zeros((total_rows, 128), F32)
        sticks = [None] * blocks
        for b in reversed(tiles):
            stick = for_own(b, jnp.exp2(scores[:, span[b]] - (sums[b][:, 0:128] + rest)))
            sticks[b] = stick.astype(BF16)
            rest = rest + sums[b][:, 128:256]
        acc = dot(jnp.concatenate(sticks, axis=1), vals)
        acc_out[:, lanes] = acc[:rows]
        rest_out[:, lanes] = rest[:rows]
        lane = lax.broadcasted_iota(jnp.int32, (rows, 64), 1)
        for d, (_, ref) in enumerate(visitors, 1):
            part = slice(d * rows, d * rows + rows)
            ref[:, lanes] = acc[part].astype(BF16)
            total = rest[part][:, 0:64]
            t1 = total.astype(BF16).astype(F32)
            t2 = (total - t1).astype(BF16).astype(F32)
            t3 = total - t1 - t2
            ref[:, 256 + h * 64 : 320 + h * 64] = jnp.where(lane == 0, t1, jnp.where(lane == 1, t2, t3)).astype(BF16)


def merge_body(acc_ref, rest_ref, m1, m2, m3, conv, w_attn, w_conv, own_out, p1, p2, p3):
    heads = []
    for h in range(2):
        lanes = slice(h * 128, h * 128 + 128)
        outside = rest_ref[:, lanes]
        total = acc_ref[:, lanes]
        for ref in (m1, m2, m3):
            total = total + jnp.exp2(-outside) * ref[:, lanes].astype(F32)
            sent = ref[:, 256 + h * 64 : 320 + h * 64].astype(F32)
            outside = outside + (sent[:, 0:1] + sent[:, 1:2] + sent[:, 2:3])
        heads.append(total.astype(BF16))
    attended = jnp.concatenate(heads, axis=1)
    convolved = conv[...]
    me = lax.axis_index("tp")
    width = own_out.shape[1] // 2
    for d, ref in enumerate((own_out, p1, p2, p3)):
        target = lax.rem(me + d, N_TP)
        columns = pl.ds(pl.multiple_of(target * width, width), width)
        ref[:, 0:width] = dot(attended, w_attn[:, columns]).astype(ref.dtype)
        ref[:, width : 2 * width] = dot(convolved, w_conv[:, columns]).astype(ref.dtype)


def gather_body(p0, p1, p2, p3, ga, gc, merged_out, stat_out):
    total = p0[...] + p1[...].astype(F32) + p2[...].astype(F32) + p3[...].astype(F32)
    branches = total.astype(BF16).astype(F32)
    width = branches.shape[1] // 2
    attn, conv = branches[:, :width], branches[:, width:]
    merged = ga[...] * attn + gc[...] * conv
    merged_out[...] = merged
    square = jnp.sum(merged * merged, axis=1, keepdims=True)
    stat_out[...] = jnp.transpose(jnp.broadcast_to(square, (square.shape[0], 128)))[0:8, :]


def final_body(merged, s0, s1, s2, s3, gain, out):
    squares = (s0[...] + s1[...] + s2[...] + s3[...]) * (1.0 / D)
    inverse = jnp.transpose(lax.rsqrt(squares + epsilon))[:, 0:1]
    out[...] = (merged[...] * inverse * gain[...]).astype(BF16)


def on_device(
    hidden_in,
    pre_gain,
    w_query,
    w_key,
    w_value,
    stick_offset,
    w_glu_a,
    w_glu_b,
    w_gate_attn,
    w_gate_conv,
    conv_taps,
    conv_bias,
    norm_gain,
    norm_shift,
    w_attn_out,
    w_conv_out,
    post_gain,
):
    def v(x):
        return ("vmem", x)

    rows = 64
    pieces = to_rotated([hidden_in] * 3)
    hidden, gain, wq, wk, wv, wga, wgb = loaded(
        (hidden_in, pre_gain.reshape(1, D), w_query, w_key, w_value, w_glu_a, w_glu_b)
    )
    wao, wco = loaded((w_attn_out, w_conv_out))
    kv, q, normed = call(
        qkv_body,
        [((8, rows, 512), BF16), ((rows, 256), BF16), ((rows, D), BF16)],
        [v(p) for p in [hidden] + pieces] + [v(gain), v(wq), v(wk), v(wv)],
        scratch=[pltpu.VMEM((rows, D), BF16)],
        flops=2 * rows * D * 768,
    )
    kv_mine = lax.all_to_all(kv, ("zl", "x"), 0, 0)
    visitors = [lax.ppermute(q, "zh", [(i, i - d) for i in range(d, N_ZH)]) for d in range(1, N_ZH)]
    gated, tail = call(
        glu_body, [((rows, 256), BF16), ((HALO, 256), BF16)], [v(normed), v(wga), v(wgb)], flops=2 * rows * D * 512
    )
    before = lax.ppermute(tail, SP, [(i, i + 1) for i in range(lax.axis_size(SP) - 1)])
    gate_a, gate_c = call(
        gates_body,
        [((rows, 512), F32), ((rows, 512), F32)],
        [v(normed)] + [("hbm", pltpu.with_memory_space_constraint(w, pltpu.HBM)) for w in (w_gate_attn, w_gate_conv)],
        scratch=[pltpu.VMEM((2, D, 512), BF16), pltpu.SemaphoreType.DMA((2 * LOAD_PARTS,))],
        flops=2 * rows * D * 1024,
    )
    convolved, stat = call(
        conv_body,
        [((rows, 256), F32), ((8, rows), F32)],
        [v(gated), v(before), v(conv_taps), v(conv_bias.reshape(1, 256))],
        scratch=[pltpu.VMEM((rows + HALO, 256), F32)],
        flops=2 * rows * 256 * 31 * 40,
    )
    stats = [stat] + to_rotated([stat] * 3)
    (conv_normed,) = call(
        conv_norm_body,
        [((rows, 256), BF16)],
        [v(convolved)]
        + [v(s) for s in stats]
        + [v(norm_gain.reshape(1, 256)), v(norm_shift.reshape(1, 256))],
        flops=2 * rows * 256 * 100,
    )
    kv_other = lax.ppermute(kv_mine, "c", [(0, 1), (1, 0)])
    acc, rest, *messages = call(
        attend_body,
        [((rows, 256), F32), ((rows, 256), F32)] + [((rows, 384), BF16)] * 3,
        [("smem", stick_offset), v(q)] + [v(x) for x in visitors] + [v(kv_mine), v(kv_other)],
        flops=2 * 2 * 256 * 1024 * 128 * 2,
    )
    returned = [lax.ppermute(m, "zh", [(i, i + d) for i in range(N_ZH - d)]) for d, m in enumerate(messages, 1)]
    partial = call(
        merge_body,
        [((rows, 1024), F32)] + [((rows, 1024), BF16)] * 3,
        [v(acc), v(rest)] + [v(m) for m in returned] + [v(conv_normed), v(wao), v(wco)],
        flops=4 * rows * 256 * D,
    )
    pieces = [partial[0]] + to_rotated(partial[1:])
    merged, square = call(
        gather_body,
        [((rows, 512), F32), ((8, rows), F32)],
        [v(x) for x in pieces] + [v(gate_a), v(gate_c)],
        flops=1000000,
    )
    squares = [square] + to_rotated([square] * 3)
    (out,) = call(
        final_body,
        [((rows, 512), BF16)],
        [v(merged)] + [v(s) for s in squares] + [v(post_gain.reshape(1, 512))],
        flops=1000000,
    )
    return out


def solution(mesh):
    torus = Mesh(mesh.devices.reshape(4, 2, 4, 2, mesh.shape["tp"]), SP_TP)

    return jax.shard_map(
        on_device,
        mesh=torus,
        in_specs=(
            P(SP_TP, None),
            P(),
            P(None, "tp"),
            P(None, "tp"),
            P(None, "tp"),
            P("tp"),
            P(None, "tp"),
            P(None, "tp"),
            P(None, "tp"),
            P(None, "tp"),
            P(None, "tp"),
            P("tp"),
            P("tp"),
            P("tp"),
            P("tp", None),
            P("tp", None),
            P("tp"),
        ),
        out_specs=P(SP, "tp"),
        check_vma=False,
    )
```

```python
import math

import jax
import jax.numpy as jnp
from jax import lax
from jax.experimental import pallas as pl
from jax.experimental.pallas import tpu as pltpu
from jax.sharding import Mesh
from jax.sharding import PartitionSpec as P

D = 2048
HEAD_DIM = 128
CONV_CH = 1024
WIDTH = 31
HALO = 32
SP = ("zh", "zl", "x", "c")
SP_TP = ("zh", "zl", "x", "c", "tp")
N_ZH = 4
N_TP = 4
LOG2E = math.log2(math.e)
BF16 = jnp.bfloat16
F32 = jnp.float32
epsilon = 1e-06
MIB = 1024 * 1024
LOAD_PARTS = 4


def dot(a, b):
    return jnp.dot(a, b, preferred_element_type=F32)


def call(body, outs, args, scratch=(), vmem=8, flops=0, out_space=jax.ShapeDtypeStruct):
    spaces = {"smem": pltpu.SMEM, "vmem": pltpu.VMEM, "hbm": pltpu.HBM}
    specs = [pl.BlockSpec(memory_space=spaces[kind]) for kind, _ in args]
    return pallas_call(body, outs, specs, args, scratch, vmem, flops, out_space)


def pallas_call(body, outs, specs, args, scratch, vmem, flops, out_space):
    return pl.pallas_call(
        body,
        out_shape=[out_space(shape, dtype) for shape, dtype in outs],
        in_specs=specs,
        out_specs=[pl.BlockSpec(memory_space=pltpu.VMEM) for _ in outs],
        scratch_shapes=list(scratch),
        compiler_params=pltpu.CompilerParams(vmem_limit_bytes=vmem * MIB),
        cost_estimate=pl.CostEstimate(flops=flops, transcendentals=0, bytes_accessed=0),
    )(*[array for _, array in args])


def to_rotated(pieces):
    return [lax.ppermute(piece, "tp", [(i, (i + d) % N_TP) for i in range(N_TP)]) for d, piece in enumerate(pieces, 1)]


def started(pairs, sems):
    copies = []
    for source, target in pairs:
        parts = LOAD_PARTS if source.shape[0] >= 256 else 1
        rows = source.shape[0] // parts
        for i in range(parts):
            part = pl.ds(i * rows, rows)
            copies.append(pltpu.make_async_copy(source.at[part], target.at[part], sems.at[len(copies)]))
    for copy in copies:
        copy.start()
    return copies


def load_body(*refs):
    count = (len(refs) - 1) // 2
    for copy in started(zip(refs[:count], refs[count:-1]), refs[-1]):
        copy.wait()


def in_hbm(x):
    return ("hbm", pltpu.with_memory_space_constraint(x, pltpu.HBM))


def loaded(arrays):
    return call(
        load_body,
        [(x.shape, x.dtype) for x in arrays],
        [in_hbm(x) for x in arrays],
        scratch=[pltpu.SemaphoreType.DMA((LOAD_PARTS * len(arrays),))],
        flops=10000000,
        out_space=pltpu.VMEM,
    )


def qkv_body(x0, x1, x2, x3, gain, wq, wk, wv, kv_out, q_out, normed_out, rows):
    me = lax.axis_index("tp")
    for d, ref in enumerate((x0, x1, x2, x3)):
        source = lax.rem(me + N_TP - d, N_TP)
        rows[pl.ds(pl.multiple_of(source * 16, 16), 16), :] = ref[...]
    values = rows[...].astype(F32)
    inverse = lax.rsqrt(jnp.mean(values * values, axis=1, keepdims=True) + epsilon)
    normed = (values * inverse * gain[...]).astype(BF16)
    normed_out[...] = normed
    keys = dot(normed, wk[...]).astype(BF16)
    vals = dot(normed, wv[...]).astype(BF16)
    for i in range(kv_out.shape[0]):
        kv_out[i, :, 0:256] = keys
        kv_out[i, :, 256:512] = vals
    q_out[...] = dot(normed, wq[...]).astype(BF16)


def glu_body(normed_ref, wa, wb, gated_out, tail_out):
    normed = normed_ref[...]
    left = dot(normed, wa[...]).astype(BF16).astype(F32)
    right = dot(normed, wb[...]).astype(BF16).astype(F32)
    gated = (left * jax.nn.sigmoid(right)).astype(BF16)
    gated_out[...] = gated
    tail_out[...] = gated[gated.shape[0] - HALO :, :]


def gates_body(normed_ref, wa, wc, ga_out, gc_out, held, sems):
    rows = D // LOAD_PARTS
    copies = []
    for i in range(LOAD_PARTS):
        part = pl.ds(i * rows, rows)
        for j, source in enumerate((wa, wc)):
            copies.append(pltpu.make_async_copy(source.at[part], held.at[j, part], sems.at[len(copies)]))
    for copy in copies:
        copy.start()
    totals = [0.0, 0.0]
    for i in range(LOAD_PARTS):
        part = slice(i * rows, i * rows + rows)
        for j in range(2):
            copies[2 * i + j].wait()
            totals[j] = totals[j] + dot(normed_ref[:, part], held[j, part, :])
    ga_out[...] = jax.nn.sigmoid(totals[0].astype(BF16).astype(F32))
    gc_out[...] = jax.nn.sigmoid(totals[1].astype(BF16).astype(F32))


def conv_body(gated_ref, tail_ref, taps, bias, conv_out, stat_out, padded):
    rows = gated_ref.shape[0]
    tail = tail_ref[...].astype(F32)
    place = ((lax.axis_index("zh") * 2 + lax.axis_index("zl")) * 4 + lax.axis_index("x")) * 2 + lax.axis_index("c")
    padded[0:HALO, :] = jnp.where(place == 0, jnp.zeros_like(tail), tail)
    padded[HALO : HALO + rows, :] = gated_ref[...].astype(F32)
    total = jnp.broadcast_to(bias[...], (rows, bias.shape[1]))
    first = HALO - (WIDTH - 1)
    for i in range(WIDTH):
        total = total + taps[i : i + 1, :] * padded[first + i : first + i + rows, :]
    conv_out[...] = total
    mean = jnp.mean(total, axis=1, keepdims=True)
    centered = total - mean
    squares = jnp.sum(centered * centered, axis=1, keepdims=True)
    lane = lax.broadcasted_iota(jnp.int32, (rows, 128), 1)
    turned = jnp.transpose(jnp.where(lane < 4, mean, squares))
    stat_out[...] = turned[0:8, :]


def conv_norm_body(conv_ref, s0, s1, s2, s3, gain, shift, normed_out):
    stats = [s[...] for s in (s0, s1, s2, s3)]
    means = [s[0:4, :] for s in stats]
    mean = (means[0] + means[1] + means[2] + means[3]) * (1.0 / N_TP)
    spread = jnp.zeros_like(mean)
    for s, m in zip(stats, means):
        spread = spread + s[4:8, :] + (m - mean) * (m - mean) * (CONV_CH // N_TP)
    inverse = lax.rsqrt(spread * (1.0 / CONV_CH) + epsilon)
    columns = jnp.transpose(jnp.concatenate([mean, inverse], axis=0))
    mean = columns[:, 0:1]
    inverse = columns[:, 4:5]
    scaled = (conv_ref[...] - mean) * inverse * gain[...] + shift[...]
    normed_out[...] = (scaled * jax.nn.sigmoid(scaled)).astype(BF16)


def attend_body(
    offset, q0, q1, q2, q3, mine, other, wa, wc, acc_out, rest_out, m1, m2, m3, wa_out, wc_out, sems
):
    copies = started(((wa, wa_out), (wc, wc_out)), sems)
    group = lax.axis_index("zh")
    visitors = ((q1, m1), (q2, m2), (q3, m3))
    for condition, count in ((group < N_ZH - 2, 3), (group == N_ZH - 2, 1), (group == N_ZH - 1, 0)):

        @pl.when(condition)
        def _():
            attend(offset, q0, visitors[:count], mine, other, acc_out, rest_out)

    for copy in copies:
        copy.wait()


def attend(offset, q0, visitors, mine, other, acc_out, rest_out):
    core = lax.axis_index("c")
    rows = q0.shape[0]
    blocks = mine.shape[0]
    total_rows = rows * (1 + len(visitors))
    position = (lax.axis_index("zl") * 4 + lax.axis_index("x")) * 128 + core * 64
    query_pos = position + lax.broadcasted_iota(jnp.int32, (rows, 128), 0)
    index = lax.broadcasted_iota(jnp.int32, (1, 128), 1)
    place = lax.rem(index + core * 64, 128)
    row_index = lax.rem(lax.broadcasted_iota(jnp.int32, (256, 256), 0), 128)
    col_index = lax.broadcasted_iota(jnp.int32, (256, 256), 1)
    row_place = lax.rem(row_index + core * 64, 128)
    col_place = lax.rem(col_index + core * 64, 128)
    suffix = jnp.where((col_index >= 128) | (row_place >= col_place), 1.0, 0.0).astype(BF16)
    scale = LOG2E / math.sqrt(HEAD_DIM)

    tiles = range(blocks)
    span = [slice(b * 128, b * 128 + 128) for b in tiles]
    own_causal = [(b * 128 + place) < query_pos for b in tiles]

    def for_own(b, x):
        masked = jnp.where(own_causal[b], x[:rows], 0.0)
        return jnp.concatenate([masked, x[rows:]], axis=0) if visitors else masked

    for h in range(2):
        lanes = slice(h * 128, h * 128 + 128)
        value_lanes = slice(256 + h * 128, 256 + h * 128 + 128)
        queries = jnp.concatenate([q[:, lanes] for q in [q0] + [q for q, _ in visitors]], axis=0)
        keys = jnp.concatenate([ref[b, :, lanes] for b in tiles for ref in (mine, other)], axis=0)
        vals = jnp.concatenate([ref[b, :, value_lanes] for b in tiles for ref in (mine, other)], axis=0)
        scores = lax.dot_general(queries, keys, (((1,), (1,)), ((), ())), preferred_element_type=F32)
        scores = scores * scale + offset[h] * LOG2E
        soft = jnp.maximum(scores, 0.0) + jnp.log2(1.0 + jnp.exp2(-jnp.abs(scores)))
        split = []
        for b in tiles:
            part = for_own(b, soft[:, span[b]])
            high = part.astype(BF16)
            low = (part - high.astype(F32)).astype(BF16)
            split.append(jnp.concatenate([high, low], axis=1))
        sums = dot(jnp.concatenate(split, axis=0), suffix)
        sums = [sums[b * total_rows : (b + 1) * total_rows] for b in tiles]
        rest = jnp.zeros((total_rows, 128), F32)
        sticks = [None] * blocks
        for b in reversed(tiles):
            stick = for_own(b, jnp.exp2(scores[:, span[b]] - (sums[b][:, 0:128] + rest)))
            sticks[b] = stick.astype(BF16)
            rest = rest + sums[b][:, 128:256]
        acc = dot(jnp.concatenate(sticks, axis=1), vals)
        acc_out[:, lanes] = acc[:rows]
        rest_out[:, lanes] = rest[:rows]
        for d, (_, ref) in enumerate(visitors, 1):
            part = slice(d * rows, d * rows + rows)
            ref[0:rows, lanes] = acc[part].astype(BF16)
            total = jnp.transpose(rest[part])[0:8, :]
            high = total.astype(BF16)
            ref[rows : rows + 8, h * 64 : h * 64 + 64] = high
            ref[rows : rows + 8, 128 + h * 64 : 192 + h * 64] = (total - high.astype(F32)).astype(BF16)


def merge_body(acc_ref, rest_ref, m1, m2, m3, conv, w_attn, w_conv, own_out, p1, p2, p3):
    rows = acc_ref.shape[0]
    messages = (m1, m2, m3)
    group = lax.axis_index("zh")
    held = [jnp.where(group >= d, ref[...].astype(F32), 0.0) for d, ref in enumerate(messages, 1)]
    sent = [x[rows : rows + 8, :] for x in held]
    totals = [x[:, h * 64 : h * 64 + 64] + x[:, 128 + h * 64 : 192 + h * 64] for x in sent for h in range(2)]
    totals = jnp.transpose(jnp.concatenate(totals, axis=0))
    heads = []
    for h in range(2):
        lanes = slice(h * 128, h * 128 + 128)
        outside = rest_ref[:, lanes]
        total = acc_ref[:, lanes]
        for d, x in enumerate(held):
            total = total + jnp.exp2(-outside) * x[0:rows, lanes]
            column = 8 * (2 * d + h)
            outside = outside + totals[:, column : column + 1]
        heads.append(total.astype(BF16))
    attended = jnp.concatenate(heads, axis=1)
    convolved = conv[...]
    me = lax.axis_index("tp")
    width = own_out.shape[1] // 2
    for d, ref in enumerate((own_out, p1, p2, p3)):
        target = lax.rem(me + d, N_TP)
        columns = pl.ds(pl.multiple_of(target * width, width), width)
        ref[:, 0:width] = dot(attended, w_attn[:, columns]).astype(ref.dtype)
        ref[:, width : 2 * width] = dot(convolved, w_conv[:, columns]).astype(ref.dtype)


def gather_body(p0, p1, p2, p3, ga, gc, merged_out, stat_out):
    total = p0[...] + p1[...].astype(F32) + p2[...].astype(F32) + p3[...].astype(F32)
    branches = total.astype(BF16).astype(F32)
    width = branches.shape[1] // 2
    attn, conv = branches[:, :width], branches[:, width:]
    merged = ga[...] * attn + gc[...] * conv
    merged_out[...] = merged
    square = jnp.sum(merged * merged, axis=1, keepdims=True)
    stat_out[...] = jnp.transpose(jnp.broadcast_to(square, (square.shape[0], 128)))[0:8, :]


def final_body(merged, s0, s1, s2, s3, gain, out):
    squares = (s0[...] + s1[...] + s2[...] + s3[...]) * (1.0 / D)
    inverse = jnp.transpose(lax.rsqrt(squares + epsilon))[:, 0:1]
    out[...] = (merged[...] * inverse * gain[...]).astype(BF16)


def on_device(
    hidden_in,
    pre_gain,
    w_query,
    w_key,
    w_value,
    stick_offset,
    w_glu_a,
    w_glu_b,
    w_gate_attn,
    w_gate_conv,
    conv_taps,
    conv_bias,
    norm_gain,
    norm_shift,
    w_attn_out,
    w_conv_out,
    post_gain,
):
    def v(x):
        return ("vmem", x)

    rows = 64
    pieces = to_rotated([hidden_in] * 3)
    hidden, gain, wq, wk, wv, wga, wgb = loaded(
        (hidden_in, pre_gain.reshape(1, D), w_query, w_key, w_value, w_glu_a, w_glu_b)
    )
    kv, q, normed = call(
        qkv_body,
        [((8, rows, 512), BF16), ((rows, 256), BF16), ((rows, D), BF16)],
        [v(p) for p in [hidden] + pieces] + [v(gain), v(wq), v(wk), v(wv)],
        scratch=[pltpu.VMEM((rows, D), BF16)],
        flops=2 * rows * D * 768,
    )
    kv_mine = lax.all_to_all(kv, ("zl", "x"), 0, 0)
    visitors = [lax.ppermute(q, "zh", [(i, i - d) for i in range(d, N_ZH)]) for d in range(1, N_ZH)]
    gated, tail = call(
        glu_body, [((rows, 256), BF16), ((HALO, 256), BF16)], [v(normed), v(wga), v(wgb)], flops=2 * rows * D * 512
    )
    count = lax.axis_size(SP)
    before = lax.ppermute(tail, SP, [(i, (i + 1) % count) for i in range(count)])
    gate_a, gate_c = call(
        gates_body,
        [((rows, 512), F32), ((rows, 512), F32)],
        [v(normed)] + [in_hbm(w) for w in (w_gate_attn, w_gate_conv)],
        scratch=[pltpu.VMEM((2, D, 512), BF16), pltpu.SemaphoreType.DMA((2 * LOAD_PARTS,))],
        flops=2 * rows * D * 1024,
    )
    convolved, stat = call(
        conv_body,
        [((rows, 256), F32), ((8, rows), F32)],
        [v(gated), v(before), v(conv_taps), v(conv_bias.reshape(1, 256))],
        scratch=[pltpu.VMEM((rows + HALO, 256), F32)],
        flops=2 * rows * 256 * 31 * 40,
    )
    stats = [stat] + to_rotated([stat] * 3)
    (conv_normed,) = call(
        conv_norm_body,
        [((rows, 256), BF16)],
        [v(convolved)]
        + [v(s) for s in stats]
        + [v(norm_gain.reshape(1, 256)), v(norm_shift.reshape(1, 256))],
        flops=2 * rows * 256 * 100,
    )
    kv_other = lax.ppermute(kv_mine, "c", [(0, 1), (1, 0)])
    acc, rest, *messages, wao, wco = call(
        attend_body,
        [((rows, 256), F32), ((rows, 256), F32)] + [((rows + 8, 256), BF16)] * 3 + [((256, D), BF16)] * 2,
        [("smem", stick_offset), v(q)]
        + [v(x) for x in visitors]
        + [v(kv_mine), v(kv_other)]
        + [in_hbm(w) for w in (w_attn_out, w_conv_out)],
        scratch=[pltpu.SemaphoreType.DMA((2 * LOAD_PARTS,))],
        flops=2 * 2 * 256 * 1024 * 128 * 2,
        out_space=pltpu.VMEM,
    )
    returned = [lax.ppermute(m, "zh", [(i, (i + d) % N_ZH) for i in range(N_ZH)]) for d, m in enumerate(messages, 1)]
    partial = call(
        merge_body,
        [((rows, 1024), F32)] + [((rows, 1024), BF16)] * 3,
        [v(acc), v(rest)] + [v(m) for m in returned] + [v(conv_normed), v(wao), v(wco)],
        flops=4 * rows * 256 * D,
    )
    pieces = [partial[0]] + to_rotated(partial[1:])
    merged, square = call(
        gather_body,
        [((rows, 512), F32), ((8, rows), F32)],
        [v(x) for x in pieces] + [v(gate_a), v(gate_c)],
        flops=1000000,
    )
    squares = [square] + to_rotated([square] * 3)
    (out,) = call(
        final_body,
        [((rows, 512), BF16)],
        [v(merged)] + [v(s) for s in squares] + [v(post_gain.reshape(1, 512))],
        flops=1000000,
    )
    return out


def solution(mesh):
    torus = Mesh(mesh.devices.reshape(4, 2, 4, 2, mesh.shape["tp"]), SP_TP)

    return jax.shard_map(
        on_device,
        mesh=torus,
        in_specs=(
            P(SP_TP, None),
            P(),
            P(None, "tp"),
            P(None, "tp"),
            P(None, "tp"),
            P("tp"),
            P(None, "tp"),
            P(None, "tp"),
            P(None, "tp"),
            P(None, "tp"),
            P(None, "tp"),
            P("tp"),
            P("tp"),
            P("tp"),
            P("tp", None),
            P("tp", None),
            P("tp"),
        ),
        out_specs=P(SP, "tp"),
        check_vma=False,
    )
```

```python
import math

import jax
import jax.numpy as jnp
from jax import lax
from jax.experimental import pallas as pl
from jax.experimental.pallas import tpu as pltpu
from jax.sharding import Mesh
from jax.sharding import PartitionSpec as P

D = 2048
HEAD_DIM = 128
CONV_CH = 1024
WIDTH = 31
HALO = 32
SP = ("zh", "zl", "x", "c")
SP_TP = ("zh", "zl", "x", "c", "tp")
N_ZH = 4
N_TP = 4
LOG2E = math.log2(math.e)
BF16 = jnp.bfloat16
F32 = jnp.float32
epsilon = 1e-06
MIB = 1024 * 1024
LOAD_PARTS = 4


def dot(a, b):
    return jnp.dot(a, b, preferred_element_type=F32)


def call(body, outs, args, scratch=(), vmem=8, flops=0, out_space=jax.ShapeDtypeStruct):
    spaces = {"smem": pltpu.SMEM, "vmem": pltpu.VMEM, "hbm": pltpu.HBM}
    specs = [pl.BlockSpec(memory_space=spaces[kind]) for kind, _ in args]
    return pallas_call(body, outs, specs, args, scratch, vmem, flops, out_space)


def pallas_call(body, outs, specs, args, scratch, vmem, flops, out_space):
    return pl.pallas_call(
        body,
        out_shape=[out_space(shape, dtype) for shape, dtype in outs],
        in_specs=specs,
        out_specs=[pl.BlockSpec(memory_space=pltpu.VMEM) for _ in outs],
        scratch_shapes=list(scratch),
        compiler_params=pltpu.CompilerParams(vmem_limit_bytes=vmem * MIB),
        cost_estimate=pl.CostEstimate(flops=flops, transcendentals=0, bytes_accessed=0),
    )(*[array for _, array in args])


def to_rotated(pieces):
    return [lax.ppermute(piece, "tp", [(i, (i + d) % N_TP) for i in range(N_TP)]) for d, piece in enumerate(pieces, 1)]


def started(pairs, sems):
    copies = []
    for source, target in pairs:
        parts = LOAD_PARTS if source.shape[0] >= 256 else 1
        rows = source.shape[0] // parts
        for i in range(parts):
            part = pl.ds(i * rows, rows)
            copies.append(pltpu.make_async_copy(source.at[part], target.at[part], sems.at[len(copies)]))
    for copy in copies:
        copy.start()
    return copies


def load_body(*refs):
    count = (len(refs) - 1) // 2
    for copy in started(zip(refs[:count], refs[count:-1]), refs[-1]):
        copy.wait()


def in_hbm(x):
    return ("hbm", pltpu.with_memory_space_constraint(x, pltpu.HBM))


def loaded(arrays):
    return call(
        load_body,
        [(x.shape, x.dtype) for x in arrays],
        [in_hbm(x) for x in arrays],
        scratch=[pltpu.SemaphoreType.DMA((LOAD_PARTS * len(arrays),))],
        flops=10000000,
        out_space=pltpu.VMEM,
    )


def qkv_body(x0, x1, x2, x3, gain, wq, wk, wv, wa, wb, kv_out, q_out, normed_out, gated_out, tail_out, rows):
    me = lax.axis_index("tp")
    for d, ref in enumerate((x0, x1, x2, x3)):
        source = lax.rem(me + N_TP - d, N_TP)
        rows[pl.ds(pl.multiple_of(source * 16, 16), 16), :] = ref[...]
    values = rows[...].astype(F32)
    inverse = lax.rsqrt(jnp.mean(values * values, axis=1, keepdims=True) + epsilon)
    normed = (values * inverse * gain[...]).astype(BF16)
    normed_out[...] = normed
    keys = dot(normed, wk[...]).astype(BF16)
    vals = dot(normed, wv[...]).astype(BF16)
    for i in range(kv_out.shape[0]):
        kv_out[i, :, 0:256] = keys
        kv_out[i, :, 256:512] = vals
    q_out[...] = dot(normed, wq[...]).astype(BF16)
    left = dot(normed, wa[...]).astype(BF16).astype(F32)
    right = dot(normed, wb[...]).astype(BF16).astype(F32)
    gated = (left * jax.nn.sigmoid(right)).astype(BF16)
    gated_out[...] = gated
    tail_out[...] = gated[gated.shape[0] - HALO :, :]


def gates_body(normed_ref, wa, wc, ga_out, gc_out):
    normed = normed_ref[...]
    ga_out[...] = jax.nn.sigmoid(dot(normed, wa[...]).astype(BF16).astype(F32))
    gc_out[...] = jax.nn.sigmoid(dot(normed, wc[...]).astype(BF16).astype(F32))


def conv_body(gated_ref, tail_ref, taps, bias, conv_out, stat_out, padded):
    rows = gated_ref.shape[0]
    tail = tail_ref[...].astype(F32)
    place = ((lax.axis_index("zh") * 2 + lax.axis_index("zl")) * 4 + lax.axis_index("x")) * 2 + lax.axis_index("c")
    padded[0:HALO, :] = jnp.where(place == 0, jnp.zeros_like(tail), tail)
    padded[HALO : HALO + rows, :] = gated_ref[...].astype(F32)
    total = jnp.broadcast_to(bias[...], (rows, bias.shape[1]))
    first = HALO - (WIDTH - 1)
    for i in range(WIDTH):
        total = total + taps[i : i + 1, :] * padded[first + i : first + i + rows, :]
    conv_out[...] = total
    mean = jnp.mean(total, axis=1, keepdims=True)
    centered = total - mean
    squares = jnp.sum(centered * centered, axis=1, keepdims=True)
    lane = lax.broadcasted_iota(jnp.int32, (rows, 128), 1)
    turned = jnp.transpose(jnp.where(lane < 4, mean, squares))
    stat_out[...] = turned[0:8, :]


def conv_norm_body(conv_ref, s0, s1, s2, s3, gain, shift, normed_out):
    stats = [s[...] for s in (s0, s1, s2, s3)]
    means = [s[0:4, :] for s in stats]
    mean = (means[0] + means[1] + means[2] + means[3]) * (1.0 / N_TP)
    spread = jnp.zeros_like(mean)
    for s, m in zip(stats, means):
        spread = spread + s[4:8, :] + (m - mean) * (m - mean) * (CONV_CH // N_TP)
    inverse = lax.rsqrt(spread * (1.0 / CONV_CH) + epsilon)
    columns = jnp.transpose(jnp.concatenate([mean, inverse], axis=0))
    mean = columns[:, 0:1]
    inverse = columns[:, 4:5]
    scaled = (conv_ref[...] - mean) * inverse * gain[...] + shift[...]
    normed_out[...] = (scaled * jax.nn.sigmoid(scaled)).astype(BF16)


def visit_body(offset, q1, q2, q3, mine, other, m1, m2, m3):
    group = lax.axis_index("zh")
    pairs = ((q1, m1), (q2, m2), (q3, m3))
    rows = q1.shape[0]
    for condition, count in ((group < N_ZH - 2, 3), (group == N_ZH - 2, 1)):

        @pl.when(condition)
        def _():
            suffix = suffix_matrix()
            for h in range(2):
                acc, rest = attend(offset, h, [q for q, _ in pairs[:count]], mine, other, suffix, False)
                for d, (_, ref) in enumerate(pairs[:count]):
                    part = slice(d * rows, d * rows + rows)
                    ref[0:rows, h * 128 : h * 128 + 128] = acc[part].astype(BF16)
                    total = jnp.transpose(rest[part])[0:8, :]
                    high = total.astype(BF16)
                    ref[rows : rows + 8, h * 64 : h * 64 + 64] = high
                    ref[rows : rows + 8, 128 + h * 64 : 192 + h * 64] = (total - high.astype(F32)).astype(BF16)


def own_body(offset, q, mine, other, acc_out, rest_out):
    suffix = suffix_matrix()
    for h in range(2):
        lanes = slice(h * 128, h * 128 + 128)
        acc_out[:, lanes], rest_out[:, lanes] = attend(offset, h, [q], mine, other, suffix, True)


def place_of(index):
    return (index + lax.axis_index("c") * 64) & 127


def suffix_matrix():
    row_place = place_of(lax.broadcasted_iota(jnp.int32, (256, 256), 0))
    column = lax.broadcasted_iota(jnp.int32, (256, 256), 1)
    return jnp.where((column >= 128) | (row_place >= place_of(column)), 1.0, 0.0).astype(BF16)


def attend(offset, h, query_refs, mine, other, suffix, own):
    core = lax.axis_index("c")
    blocks = mine.shape[0]
    rows = sum(q.shape[0] for q in query_refs)
    place = place_of(lax.broadcasted_iota(jnp.int32, (1, 128), 1))
    position = (lax.axis_index("zl") * 4 + lax.axis_index("x")) * 128 + core * 64
    query_pos = position + lax.broadcasted_iota(jnp.int32, (rows, 128), 0)
    tiles = range(blocks)
    span = [slice(b * 128, b * 128 + 128) for b in tiles]
    lanes = slice(h * 128, h * 128 + 128)
    value_lanes = slice(256 + h * 128, 256 + h * 128 + 128)

    def causal(b, x):
        return jnp.where((b * 128 + place) < query_pos, x, 0.0) if own else x

    queries = jnp.concatenate([q[:, lanes] for q in query_refs], axis=0)
    keys = jnp.concatenate([ref[b, :, lanes] for b in tiles for ref in (mine, other)], axis=0)
    vals = jnp.concatenate([ref[b, :, value_lanes] for b in tiles for ref in (mine, other)], axis=0)
    scores = lax.dot_general(queries, keys, (((1,), (1,)), ((), ())), preferred_element_type=F32)
    scores = scores * (LOG2E / math.sqrt(HEAD_DIM)) + offset[h] * LOG2E
    soft = jnp.maximum(scores, 0.0) + jnp.log2(1.0 + jnp.exp2(-jnp.abs(scores)))
    split = []
    for b in tiles:
        part = causal(b, soft[:, span[b]])
        high = part.astype(BF16)
        low = (part - high.astype(F32)).astype(BF16)
        split.append(jnp.concatenate([high, low], axis=1))
    sums = dot(jnp.concatenate(split, axis=0), suffix)
    sums = [sums[b * rows : (b + 1) * rows] for b in tiles]
    rest = jnp.zeros((rows, 128), F32)
    sticks = [None] * blocks
    for b in reversed(tiles):
        stick = causal(b, jnp.exp2(scores[:, span[b]] - (sums[b][:, 0:128] + rest)))
        sticks[b] = stick.astype(BF16)
        rest = rest + sums[b][:, 128:256]
    return dot(jnp.concatenate(sticks, axis=1), vals), rest


def merge_body(acc_ref, rest_ref, m1, m2, m3, conv, w_attn, w_conv, own_out, p1, p2, p3):
    rows = acc_ref.shape[0]
    messages = (m1, m2, m3)
    group = lax.axis_index("zh")
    held = [jnp.where(group >= d, ref[...].astype(F32), 0.0) for d, ref in enumerate(messages, 1)]
    sent = [x[rows : rows + 8, :] for x in held]
    totals = [x[:, h * 64 : h * 64 + 64] + x[:, 128 + h * 64 : 192 + h * 64] for x in sent for h in range(2)]
    totals = jnp.transpose(jnp.concatenate(totals, axis=0))
    heads = []
    for h in range(2):
        lanes = slice(h * 128, h * 128 + 128)
        outside = rest_ref[:, lanes]
        total = acc_ref[:, lanes]
        for d, x in enumerate(held):
            total = total + jnp.exp2(-outside) * x[0:rows, lanes]
            column = 8 * (2 * d + h)
            outside = outside + totals[:, column : column + 1]
        heads.append(total.astype(BF16))
    attended = jnp.concatenate(heads, axis=1)
    convolved = conv[...]
    me = lax.axis_index("tp")
    width = own_out.shape[1] // 2
    for d, ref in enumerate((own_out, p1, p2, p3)):
        target = lax.rem(me + d, N_TP)
        columns = pl.ds(pl.multiple_of(target * width, width), width)
        ref[:, 0:width] = dot(attended, w_attn[:, columns]).astype(ref.dtype)
        ref[:, width : 2 * width] = dot(convolved, w_conv[:, columns]).astype(ref.dtype)


def gather_body(p0, p1, p2, p3, ga, gc, merged_out, stat_out):
    total = p0[...] + p1[...].astype(F32) + p2[...].astype(F32) + p3[...].astype(F32)
    branches = total.astype(BF16).astype(F32)
    width = branches.shape[1] // 2
    attn, conv = branches[:, :width], branches[:, width:]
    merged = ga[...] * attn + gc[...] * conv
    merged_out[...] = merged
    square = jnp.sum(merged * merged, axis=1, keepdims=True)
    stat_out[...] = jnp.transpose(jnp.broadcast_to(square, (square.shape[0], 128)))[0:8, :]


def final_body(merged, s0, s1, s2, s3, gain, out):
    squares = (s0[...] + s1[...] + s2[...] + s3[...]) * (1.0 / D)
    inverse = jnp.transpose(lax.rsqrt(squares + epsilon))[:, 0:1]
    out[...] = (merged[...] * inverse * gain[...]).astype(BF16)


def on_device(
    hidden_in,
    pre_gain,
    w_query,
    w_key,
    w_value,
    stick_offset,
    w_glu_a,
    w_glu_b,
    w_gate_attn,
    w_gate_conv,
    conv_taps,
    conv_bias,
    norm_gain,
    norm_shift,
    w_attn_out,
    w_conv_out,
    post_gain,
):
    def v(x):
        return ("vmem", x)

    rows = 64
    pieces = to_rotated([hidden_in] * 3)
    hidden, gain, wq, wk, wv, wga, wgb = loaded(
        (hidden_in, pre_gain.reshape(1, D), w_query, w_key, w_value, w_glu_a, w_glu_b)
    )
    kv, q, normed, gated, tail = call(
        qkv_body,
        [((8, rows, 512), BF16), ((rows, 256), BF16), ((rows, D), BF16), ((rows, 256), BF16), ((HALO, 256), BF16)],
        [v(p) for p in [hidden] + pieces] + [v(gain), v(wq), v(wk), v(wv), v(wga), v(wgb)],
        scratch=[pltpu.VMEM((rows, D), BF16)],
        flops=2 * rows * D * 768,
    )
    kv_mine = lax.all_to_all(kv, ("zl", "x"), 0, 0)
    visitors = [lax.ppermute(q, "zh", [(i, i - d) for i in range(d, N_ZH)]) for d in range(1, N_ZH)]
    count = lax.axis_size(SP)
    before = lax.ppermute(tail, SP, [(i, (i + 1) % count) for i in range(count)])
    gate_a, gate_c = call(
        gates_body,
        [((rows, 512), F32), ((rows, 512), F32)],
        [v(normed), v(w_gate_attn), v(w_gate_conv)],
        flops=2 * rows * D * 1024,
    )
    convolved, stat = call(
        conv_body,
        [((rows, 256), F32), ((8, rows), F32)],
        [v(gated), v(before), v(conv_taps), v(conv_bias.reshape(1, 256))],
        scratch=[pltpu.VMEM((rows + HALO, 256), F32)],
        flops=2 * rows * 256 * 31 * 40,
    )
    stats = [stat] + to_rotated([stat] * 3)
    (conv_normed,) = call(
        conv_norm_body,
        [((rows, 256), BF16)],
        [v(convolved)]
        + [v(s) for s in stats]
        + [v(norm_gain.reshape(1, 256)), v(norm_shift.reshape(1, 256))],
        flops=2 * rows * 256 * 100,
    )
    kv_other = lax.ppermute(kv_mine, "c", [(0, 1), (1, 0)])
    messages = call(
        visit_body,
        [((rows + 8, 256), BF16)] * 3,
        [("smem", stick_offset)] + [v(x) for x in visitors] + [v(kv_mine), v(kv_other)],
        flops=2 * 2 * 192 * 1024 * 128 * 2,
    )
    acc, rest = call(
        own_body,
        [((rows, 256), F32), ((rows, 256), F32)],
        [("smem", stick_offset), v(q), v(kv_mine), v(kv_other)],
        flops=2 * 2 * 64 * 1024 * 128 * 2,
    )
    returned = [lax.ppermute(m, "zh", [(i, (i + d) % N_ZH) for i in range(N_ZH)]) for d, m in enumerate(messages, 1)]
    partial = call(
        merge_body,
        [((rows, 1024), F32)] + [((rows, 1024), BF16)] * 3,
        [v(acc), v(rest)] + [v(m) for m in returned] + [v(conv_normed), v(w_attn_out), v(w_conv_out)],
        flops=4 * rows * 256 * D,
    )
    pieces = [partial[0]] + to_rotated(partial[1:])
    merged, square = call(
        gather_body,
        [((rows, 512), F32), ((8, rows), F32)],
        [v(x) for x in pieces] + [v(gate_a), v(gate_c)],
        flops=1000000,
    )
    squares = [square] + to_rotated([square] * 3)
    (out,) = call(
        final_body,
        [((rows, 512), BF16)],
        [v(merged)] + [v(s) for s in squares] + [v(post_gain.reshape(1, 512))],
        flops=1000000,
    )
    return out


def solution(mesh):
    torus = Mesh(mesh.devices.reshape(4, 2, 4, 2, mesh.shape["tp"]), SP_TP)

    return jax.shard_map(
        on_device,
        mesh=torus,
        in_specs=(
            P(SP_TP, None),
            P(),
            P(None, "tp"),
            P(None, "tp"),
            P(None, "tp"),
            P("tp"),
            P(None, "tp"),
            P(None, "tp"),
            P(None, "tp"),
            P(None, "tp"),
            P(None, "tp"),
            P("tp"),
            P("tp"),
            P("tp"),
            P("tp", None),
            P("tp", None),
            P("tp"),
        ),
        out_specs=P(SP, "tp"),
        check_vma=False,
    )
```

```python
import math

import jax
import jax.numpy as jnp
from jax import lax
from jax.experimental import pallas as pl
from jax.experimental.pallas import tpu as pltpu
from jax.sharding import Mesh
from jax.sharding import PartitionSpec as P

D = 2048
HEAD_DIM = 128
CONV_CH = 1024
WIDTH = 31
HALO = 32
SP = ("zh", "zl", "x", "c")
SP_TP = ("zh", "zl", "x", "c", "tp")
N_ZH = 4
N_TP = 4
LOG2E = math.log2(math.e)
BF16 = jnp.bfloat16
F32 = jnp.float32
epsilon = 1e-06
MIB = 1024 * 1024
LOAD_PARTS = 4


def dot(a, b):
    return jnp.dot(a, b, preferred_element_type=F32)


def call(body, outs, args, scratch=(), vmem=8, flops=0, out_space=jax.ShapeDtypeStruct):
    spaces = {"smem": pltpu.SMEM, "vmem": pltpu.VMEM, "hbm": pltpu.HBM}
    specs = [pl.BlockSpec(memory_space=spaces[kind]) for kind, _ in args]
    return pallas_call(body, outs, specs, args, scratch, vmem, flops, out_space)


def pallas_call(body, outs, specs, args, scratch, vmem, flops, out_space):
    return pl.pallas_call(
        body,
        out_shape=[out_space(shape, dtype) for shape, dtype in outs],
        in_specs=specs,
        out_specs=[pl.BlockSpec(memory_space=pltpu.VMEM) for _ in outs],
        scratch_shapes=list(scratch),
        compiler_params=pltpu.CompilerParams(vmem_limit_bytes=vmem * MIB),
        cost_estimate=pl.CostEstimate(flops=flops, transcendentals=0, bytes_accessed=0),
    )(*[array for _, array in args])


def to_rotated(pieces):
    return [lax.ppermute(piece, "tp", [(i, (i + d) % N_TP) for i in range(N_TP)]) for d, piece in enumerate(pieces, 1)]


def started(pairs, sems):
    copies = []
    for source, target in pairs:
        parts = LOAD_PARTS if source.shape[0] >= 256 else 1
        rows = source.shape[0] // parts
        for i in range(parts):
            part = pl.ds(i * rows, rows)
            copies.append(pltpu.make_async_copy(source.at[part], target.at[part], sems.at[len(copies)]))
    for copy in copies:
        copy.start()
    return copies


def load_body(*refs):
    count = (len(refs) - 1) // 2
    for copy in started(zip(refs[:count], refs[count:-1]), refs[-1]):
        copy.wait()


def in_hbm(x):
    return ("hbm", pltpu.with_memory_space_constraint(x, pltpu.HBM))


def loaded(arrays):
    return call(
        load_body,
        [(x.shape, x.dtype) for x in arrays],
        [in_hbm(x) for x in arrays],
        scratch=[pltpu.SemaphoreType.DMA((LOAD_PARTS * len(arrays),))],
        flops=10000000,
        out_space=pltpu.VMEM,
    )


def qkv_body(x0, x1, x2, x3, gain, wq, wk, wv, wa, wb, kv_out, q_out, normed_out, gated_out, tail_out, rows):
    me = lax.axis_index("tp")
    for d, ref in enumerate((x0, x1, x2, x3)):
        source = lax.rem(me + N_TP - d, N_TP)
        rows[pl.ds(pl.multiple_of(source * 16, 16), 16), :] = ref[...]
    values = rows[...].astype(F32)
    inverse = lax.rsqrt(jnp.mean(values * values, axis=1, keepdims=True) + epsilon)
    normed = (values * inverse * gain[...]).astype(BF16)
    normed_out[...] = normed
    keys = dot(normed, wk[...]).astype(BF16)
    vals = dot(normed, wv[...]).astype(BF16)
    for i in range(kv_out.shape[0]):
        kv_out[i, :, 0:256] = keys
        kv_out[i, :, 256:512] = vals
    q_out[...] = dot(normed, wq[...]).astype(BF16)
    left = dot(normed, wa[...]).astype(BF16).astype(F32)
    right = dot(normed, wb[...]).astype(BF16).astype(F32)
    gated = (left * jax.nn.sigmoid(right)).astype(BF16)
    gated_out[...] = gated
    tail_out[...] = gated[gated.shape[0] - HALO :, :]


def gates_body(normed_ref, wa, wc, ga_out, gc_out):
    normed = normed_ref[...]
    ga_out[...] = jax.nn.sigmoid(dot(normed, wa[...]).astype(BF16).astype(F32))
    gc_out[...] = jax.nn.sigmoid(dot(normed, wc[...]).astype(BF16).astype(F32))


def conv_body(gated_ref, tail_ref, taps, bias, conv_out, stat_out, padded):
    rows = gated_ref.shape[0]
    tail = tail_ref[...].astype(F32)
    place = ((lax.axis_index("zh") * 2 + lax.axis_index("zl")) * 4 + lax.axis_index("x")) * 2 + lax.axis_index("c")
    padded[0:HALO, :] = jnp.where(place == 0, jnp.zeros_like(tail), tail)
    padded[HALO : HALO + rows, :] = gated_ref[...].astype(F32)
    total = jnp.broadcast_to(bias[...], (rows, bias.shape[1]))
    first = HALO - (WIDTH - 1)
    for shift in range(8):
        span = rows if shift == 0 else rows + 8
        part = 0.0
        for i in range(WIDTH):
            if (first + i) % 8 == shift:
                start = first + i - shift
                part = part + taps[i : i + 1, :] * padded[start : start + span, :]
        total = total + part[shift : shift + rows, :]
    conv_out[...] = total
    mean = jnp.mean(total, axis=1, keepdims=True)
    centered = total - mean
    squares = jnp.sum(centered * centered, axis=1, keepdims=True)
    lane = lax.broadcasted_iota(jnp.int32, (rows, 128), 1)
    turned = jnp.transpose(jnp.where(lane < 4, mean, squares))
    stat_out[...] = turned[0:8, :]


def conv_norm_body(conv_ref, s0, s1, s2, s3, gain, shift, normed_out):
    stats = [s[...] for s in (s0, s1, s2, s3)]
    means = [s[0:4, :] for s in stats]
    mean = (means[0] + means[1] + means[2] + means[3]) * (1.0 / N_TP)
    spread = jnp.zeros_like(mean)
    for s, m in zip(stats, means):
        spread = spread + s[4:8, :] + (m - mean) * (m - mean) * (CONV_CH // N_TP)
    inverse = lax.rsqrt(spread * (1.0 / CONV_CH) + epsilon)
    columns = jnp.transpose(jnp.concatenate([mean, inverse], axis=0))
    mean = columns[:, 0:1]
    inverse = columns[:, 4:5]
    scaled = (conv_ref[...] - mean) * inverse * gain[...] + shift[...]
    normed_out[...] = (scaled * jax.nn.sigmoid(scaled)).astype(BF16)


def visit_body(offset, q1, q2, q3, mine, other, m1, m2, m3):
    group = lax.axis_index("zh")
    pairs = ((q1, m1), (q2, m2), (q3, m3))
    rows = q1.shape[0]
    for condition, count in ((group < N_ZH - 2, 3), (group == N_ZH - 2, 1)):

        @pl.when(condition)
        def _():
            suffix = suffix_matrix()
            for h in range(2):
                acc, rest = attend(offset, h, [q for q, _ in pairs[:count]], mine, other, suffix, False)
                for d, (_, ref) in enumerate(pairs[:count]):
                    part = slice(d * rows, d * rows + rows)
                    ref[0:rows, h * 128 : h * 128 + 128] = acc[part].astype(BF16)
                    total = jnp.transpose(rest[part])[0:8, :]
                    high = total.astype(BF16)
                    ref[rows : rows + 8, h * 64 : h * 64 + 64] = high
                    ref[rows : rows + 8, 128 + h * 64 : 192 + h * 64] = (total - high.astype(F32)).astype(BF16)


def own_body(offset, q, mine, other, acc_out, rest_out):
    suffix = suffix_matrix()
    for h in range(2):
        lanes = slice(h * 128, h * 128 + 128)
        acc_out[:, lanes], rest_out[:, lanes] = attend(offset, h, [q], mine, other, suffix, True)


def place_of(index):
    return (index + lax.axis_index("c") * 64) & 127


def suffix_matrix():
    row_place = place_of(lax.broadcasted_iota(jnp.int32, (256, 256), 0))
    column = lax.broadcasted_iota(jnp.int32, (256, 256), 1)
    return jnp.where((column >= 128) | (row_place >= place_of(column)), 1.0, 0.0).astype(BF16)


def attend(offset, h, query_refs, mine, other, suffix, own):
    core = lax.axis_index("c")
    blocks = mine.shape[0]
    rows = sum(q.shape[0] for q in query_refs)
    place = place_of(lax.broadcasted_iota(jnp.int32, (1, 128), 1))
    position = (lax.axis_index("zl") * 4 + lax.axis_index("x")) * 128 + core * 64
    query_pos = position + lax.broadcasted_iota(jnp.int32, (rows, 128), 0)
    tiles = range(blocks)
    span = [slice(b * 128, b * 128 + 128) for b in tiles]
    lanes = slice(h * 128, h * 128 + 128)
    value_lanes = slice(256 + h * 128, 256 + h * 128 + 128)

    def causal(b, x):
        return jnp.where((b * 128 + place) < query_pos, x, 0.0) if own else x

    queries = jnp.concatenate([q[:, lanes] for q in query_refs], axis=0)
    keys = jnp.concatenate([ref[b, :, lanes] for b in tiles for ref in (mine, other)], axis=0)
    vals = jnp.concatenate([ref[b, :, value_lanes] for b in tiles for ref in (mine, other)], axis=0)
    scores = lax.dot_general(queries, keys, (((1,), (1,)), ((), ())), preferred_element_type=F32)
    scores = scores * (LOG2E / math.sqrt(HEAD_DIM)) + offset[h] * LOG2E
    soft = jnp.maximum(scores, 0.0) + jnp.log2(1.0 + jnp.exp2(-jnp.abs(scores)))
    split = []
    for b in tiles:
        part = causal(b, soft[:, span[b]])
        high = part.astype(BF16)
        low = (part - high.astype(F32)).astype(BF16)
        split.append(jnp.concatenate([high, low], axis=1))
    sums = dot(jnp.concatenate(split, axis=0), suffix)
    sums = [sums[b * rows : (b + 1) * rows] for b in tiles]
    rest = jnp.zeros((rows, 128), F32)
    sticks = [None] * blocks
    for b in reversed(tiles):
        stick = causal(b, jnp.exp2(scores[:, span[b]] - (sums[b][:, 0:128] + rest)))
        sticks[b] = stick.astype(BF16)
        rest = rest + sums[b][:, 128:256]
    return dot(jnp.concatenate(sticks, axis=1), vals), rest


def merge_body(acc_ref, rest_ref, m1, m2, m3, conv, w_attn, w_conv, own_out, p1, p2, p3):
    rows = acc_ref.shape[0]
    messages = (m1, m2, m3)
    group = lax.axis_index("zh")
    held = [jnp.where(group >= d, ref[...].astype(F32), 0.0) for d, ref in enumerate(messages, 1)]
    sent = [x[rows : rows + 8, :] for x in held]
    totals = [x[:, h * 64 : h * 64 + 64] + x[:, 128 + h * 64 : 192 + h * 64] for x in sent for h in range(2)]
    totals = jnp.transpose(jnp.concatenate(totals, axis=0))
    heads = []
    for h in range(2):
        lanes = slice(h * 128, h * 128 + 128)
        outside = rest_ref[:, lanes]
        total = acc_ref[:, lanes]
        for d, x in enumerate(held):
            total = total + jnp.exp2(-outside) * x[0:rows, lanes]
            column = 8 * (2 * d + h)
            outside = outside + totals[:, column : column + 1]
        heads.append(total.astype(BF16))
    attended = jnp.concatenate(heads, axis=1)
    convolved = conv[...]
    me = lax.axis_index("tp")
    width = own_out.shape[1] // 2
    for d, ref in enumerate((own_out, p1, p2, p3)):
        target = lax.rem(me + d, N_TP)
        columns = pl.ds(pl.multiple_of(target * width, width), width)
        ref[:, 0:width] = dot(attended, w_attn[:, columns]).astype(ref.dtype)
        ref[:, width : 2 * width] = dot(convolved, w_conv[:, columns]).astype(ref.dtype)


def gather_body(p0, p1, p2, p3, ga, gc, merged_out, stat_out):
    total = p0[...] + p1[...].astype(F32) + p2[...].astype(F32) + p3[...].astype(F32)
    branches = total.astype(BF16).astype(F32)
    width = branches.shape[1] // 2
    attn, conv = branches[:, :width], branches[:, width:]
    merged = ga[...] * attn + gc[...] * conv
    merged_out[...] = merged
    square = jnp.sum(merged * merged, axis=1, keepdims=True)
    stat_out[...] = jnp.transpose(jnp.broadcast_to(square, (square.shape[0], 128)))[0:8, :]


def final_body(merged, s0, s1, s2, s3, gain, out):
    squares = (s0[...] + s1[...] + s2[...] + s3[...]) * (1.0 / D)
    inverse = jnp.transpose(lax.rsqrt(squares + epsilon))[:, 0:1]
    out[...] = (merged[...] * inverse * gain[...]).astype(BF16)


def on_device(
    hidden_in,
    pre_gain,
    w_query,
    w_key,
    w_value,
    stick_offset,
    w_glu_a,
    w_glu_b,
    w_gate_attn,
    w_gate_conv,
    conv_taps,
    conv_bias,
    norm_gain,
    norm_shift,
    w_attn_out,
    w_conv_out,
    post_gain,
):
    def v(x):
        return ("vmem", x)

    rows = 64
    pieces = to_rotated([hidden_in] * 3)
    hidden, gain, wq, wk, wv, wga, wgb = loaded(
        (hidden_in, pre_gain.reshape(1, D), w_query, w_key, w_value, w_glu_a, w_glu_b)
    )
    kv, q, normed, gated, tail = call(
        qkv_body,
        [((8, rows, 512), BF16), ((rows, 256), BF16), ((rows, D), BF16), ((rows, 256), BF16), ((HALO, 256), BF16)],
        [v(p) for p in [hidden] + pieces] + [v(gain), v(wq), v(wk), v(wv), v(wga), v(wgb)],
        scratch=[pltpu.VMEM((rows, D), BF16)],
        flops=2 * rows * D * 768,
    )
    kv_mine = lax.all_to_all(kv, ("zl", "x"), 0, 0)
    visitors = [lax.ppermute(q, "zh", [(i, i - d) for i in range(d, N_ZH)]) for d in range(1, N_ZH)]
    count = lax.axis_size(SP)
    before = lax.ppermute(tail, SP, [(i, (i + 1) % count) for i in range(count)])
    gate_a, gate_c = call(
        gates_body,
        [((rows, 512), F32), ((rows, 512), F32)],
        [v(normed), v(w_gate_attn), v(w_gate_conv)],
        flops=2 * rows * D * 1024,
    )
    convolved, stat = call(
        conv_body,
        [((rows, 256), F32), ((8, rows), F32)],
        [v(gated), v(before), v(conv_taps), v(conv_bias.reshape(1, 256))],
        scratch=[pltpu.VMEM((rows + HALO, 256), F32)],
        flops=2 * rows * 256 * 31 * 40,
    )
    stats = [stat] + to_rotated([stat] * 3)
    (conv_normed,) = call(
        conv_norm_body,
        [((rows, 256), BF16)],
        [v(convolved)]
        + [v(s) for s in stats]
        + [v(norm_gain.reshape(1, 256)), v(norm_shift.reshape(1, 256))],
        flops=2 * rows * 256 * 100,
    )
    kv_other = lax.ppermute(kv_mine, "c", [(0, 1), (1, 0)])
    messages = call(
        visit_body,
        [((rows + 8, 256), BF16)] * 3,
        [("smem", stick_offset)] + [v(x) for x in visitors] + [v(kv_mine), v(kv_other)],
        flops=2 * 2 * 192 * 1024 * 128 * 2,
    )
    acc, rest = call(
        own_body,
        [((rows, 256), F32), ((rows, 256), F32)],
        [("smem", stick_offset), v(q), v(kv_mine), v(kv_other)],
        flops=2 * 2 * 64 * 1024 * 128 * 2,
    )
    returned = [lax.ppermute(m, "zh", [(i, (i + d) % N_ZH) for i in range(N_ZH)]) for d, m in enumerate(messages, 1)]
    partial = call(
        merge_body,
        [((rows, 1024), F32)] + [((rows, 1024), BF16)] * 3,
        [v(acc), v(rest)] + [v(m) for m in returned] + [v(conv_normed), v(w_attn_out), v(w_conv_out)],
        flops=4 * rows * 256 * D,
    )
    pieces = [partial[0]] + to_rotated(partial[1:])
    merged, square = call(
        gather_body,
        [((rows, 512), F32), ((8, rows), F32)],
        [v(x) for x in pieces] + [v(gate_a), v(gate_c)],
        flops=1000000,
    )
    squares = [square] + to_rotated([square] * 3)
    (out,) = call(
        final_body,
        [((rows, 512), BF16)],
        [v(merged)] + [v(s) for s in squares] + [v(post_gain.reshape(1, 512))],
        flops=1000000,
    )
    return out


def solution(mesh):
    torus = Mesh(mesh.devices.reshape(4, 2, 4, 2, mesh.shape["tp"]), SP_TP)

    return jax.shard_map(
        on_device,
        mesh=torus,
        in_specs=(
            P(SP_TP, None),
            P(),
            P(None, "tp"),
            P(None, "tp"),
            P(None, "tp"),
            P("tp"),
            P(None, "tp"),
            P(None, "tp"),
            P(None, "tp"),
            P(None, "tp"),
            P(None, "tp"),
            P("tp"),
            P("tp"),
            P("tp"),
            P("tp", None),
            P("tp", None),
            P("tp"),
        ),
        out_specs=P(SP, "tp"),
        check_vma=False,
    )
```
